32 devices in a mesh: grp: 2 (over y), fs: 4 (over z), tp: 4 (over x, core).
Axes of the slice: x: 2, y: 2, z: 4, core: 2. Of those that a mesh axis runs over, the one named last changes fastest.
Arguments:
- tokens: bfloat16 [3072, 2048], P(('grp', 'fs'), 'tp'), parts along dimension 0, may hold values from -6 to 6
- norm_gain: float32 [2048], P('fs'), may hold values from 0.1 to 1.9
- gate_weight: float32 [4, 2048, 1024], P(None, 'fs', 'tp'), may hold values from -0.125 to 0.125
- up_weight: float32 [4, 2048, 1024], P(None, 'fs', 'tp'), may hold values from -0.125 to 0.125
- down_weight: float32 [4, 2048, 1024], P(None, 'fs', 'tp'), may hold values from -0.5 to 0.5
- expert_ids: int32 [3072, 2], P(('grp', 'fs')), parts along dimension 0, may hold values from 0 to 3, as said below
- group_logits: float32 [3072, 2], P(('grp', 'fs')), parts along dimension 0, may hold values from -2.5 to 2.5
- pair_logits: float32 [3072, 2], P(('grp', 'fs')), parts along dimension 0, may hold values from -2.5 to 2.5
Outputs:
- mixed: bfloat16 [3072, 2048], P(('grp', 'fs'), 'tp'), parts along dimension 0
- gate_out: bfloat16 [8, 2048, 1024], P(('grp', 'fs'), None, 'tp'), parts along dimension 0
- up_out: bfloat16 [8, 2048, 1024], P(('grp', 'fs'), None, 'tp'), parts along dimension 0
- down_out: bfloat16 [8, 2048, 1024], P(('grp', 'fs'), None, 'tp'), parts along dimension 0
The draws below stay inside these ranges and needn't reach their ends.
There are 2 independent parts, one for each index of `grp`. The reference program is written for one: setup_inputs(seed, part) draws one part's arguments, and reference() takes and returns one part's arrays. A program takes and returns all parts, laid end to end along the dimension named above; an argument that names none is the same for every part. Nothing has to cross between parts.
Inputs may be any that keep to these rules, and one draw needn't show every extreme that they name: `expert_ids`: each row names two different experts of one group: both ids lie in the same run of 2 consecutive ids.
All inputs are finite; a program needn't handle non-finite values.
Results may differ from the reference program's by a relative error of at most 0.015.
Values may be sent and summed in bfloat16 or wider, within the bound.
A program may use at most 64 MiB of HBM per device.

```python
from functools import partial
import jax
import jax.numpy as jnp
from jax import lax

D = 2048
FF = 1024
GROUPS = 2
TOP = 2
TOK_DEV = 384
EXPERTS = 4
EXP_GROUP = 2
CAP = 240
TOKENS = 1536
N_FS = 4
N_TP = 4


def pick_by_weight(key, table):
    running = jnp.cumsum(table, axis=1)
    total = running[:, -1]
    draw = jax.random.randint(key, (table.shape[0],), 0, 1 << 30) % total
    return jnp.sum((running <= draw[:, None]).astype(jnp.int32), axis=1).astype(jnp.int32)


def draw_expert_ids(key, part):
    base = jax.random.fold_in(key, 11)
    key_hot, key_first, key_second = jax.random.split(base, 3)
    block_count = TOKENS // TOK_DEV
    block_keys = jax.random.split(key_hot, block_count)
    orders = jax.vmap(lambda single: jax.random.permutation(single, EXPERTS))(block_keys)
    block_table = 1 + 2 * (orders < EXPERTS // 2).astype(jnp.int32)
    token_block = jnp.arange(TOKENS, dtype=jnp.int32) // TOK_DEV
    token_table = block_table[token_block]
    first_pick = pick_by_weight(key_first, token_table)
    columns = jnp.arange(EXPERTS, dtype=jnp.int32)
    allowed = (columns[None, :] // EXP_GROUP == (first_pick // EXP_GROUP)[:, None]) & (columns[None, :] != first_pick[:, None])
    second_table = token_table * allowed.astype(jnp.int32)
    second_pick = pick_by_weight(key_second, second_table)
    return jnp.stack([first_pick, second_pick], axis=1).astype(jnp.int32)


def draw_tokens(key, part):
    base = jax.random.fold_in(key, 21)
    raw = jnp.clip(jax.random.normal(base, (TOKENS, D), jnp.float32), -3.0, 3.0)
    factor = 1.0 / jnp.sqrt(jnp.mean(raw * raw, axis=1, keepdims=True) + 1e-06)
    return jnp.clip(raw * factor, -6.0, 6.0).astype(jnp.bfloat16)


def draw_group_logits(key, part):
    base = jax.random.fold_in(key, 31)
    values = jnp.clip(0.6 * jax.random.normal(base, (TOKENS, GROUPS), jnp.float32), -2.5, 2.5)
    return values.astype(jnp.float32)


def draw_pair_logits(key, part):
    base = jax.random.fold_in(key, 41)
    values = jnp.clip(0.6 * jax.random.normal(base, (TOKENS, TOP), jnp.float32), -2.5, 2.5)
    return values.astype(jnp.float32)


def shard_levels(key, shape, cuts, low, high):
    def one(axis_at, blocks):
        steps = jax.random.uniform(jax.random.fold_in(jax.random.fold_in(key, 6), axis_at), (blocks,), jnp.float32, low / len(cuts), high / len(cuts))
        return jnp.repeat(jnp.exp(steps), shape[axis_at] // blocks).reshape((-1,) + (1,) * (len(shape) - axis_at - 1))

    level = one(*cuts[0])
    for cut in cuts[1:]:
        level = level * one(*cut)
    return level


def bell_draw(rng, extent, scale, most, cuts=(), kind=jnp.bfloat16):
    values = jax.random.normal(rng, extent, jnp.float32) * scale
    if len(cuts) > 0:
        values = shard_levels(rng, extent, cuts, -0.22, 0.18) * values
    return jnp.clip(values, min=-most, max=most).astype(kind)


def setup_inputs(seed: int = 0, part: int = 0) -> dict:
    key_of = jax.random.split(jax.random.key(seed), 9)
    own_keys = jax.random.split(jax.random.fold_in(key_of[8], part), 9)
    tokens = draw_tokens(jax.random.fold_in(jax.random.fold_in(key_of[8], part), 71), part)
    norm_gain = jnp.clip(1.0 + 0.18 * jax.random.normal(key_of[1], (D,), jnp.float32), 0.1, 1.9)
    gate_weight = bell_draw(key_of[2], (EXPERTS, D, FF), D ** -0.5, 0.125, ((1, 4), (2, 4)), jnp.float32)
    up_weight = bell_draw(key_of[3], (EXPERTS, D, FF), D ** -0.5, 0.125, ((1, 4), (2, 4)), jnp.float32)
    down_weight = bell_draw(key_of[4], (EXPERTS, D, FF), (FF // 8) ** -0.5, 0.5, ((1, 4), (2, 4)), jnp.float32)
    expert_ids = draw_expert_ids(jax.random.fold_in(jax.random.fold_in(key_of[8], part), 71), part)
    group_logits = draw_group_logits(jax.random.fold_in(jax.random.fold_in(key_of[8], part), 71), part)
    pair_logits = draw_pair_logits(jax.random.fold_in(jax.random.fold_in(key_of[8], part), 71), part)
    return dict(tokens=tokens, norm_gain=norm_gain, gate_weight=gate_weight, up_weight=up_weight, down_weight=down_weight, expert_ids=expert_ids, group_logits=group_logits, pair_logits=pair_logits)


def routing(block_ids, experts, capacity):
    entries = block_ids.reshape(-1).astype(jnp.int32)
    onehot = (entries[:, None] == jnp.arange(experts, dtype=jnp.int32)[None, :]).astype(jnp.int32)
    before = jnp.cumsum(onehot, axis=0) - onehot
    entry_rank = jnp.sum(before * onehot, axis=1)
    kept = entry_rank < capacity
    slot_index = jnp.where(kept, entries * capacity + entry_rank, experts * capacity)
    return slot_index.astype(jnp.int32), kept


def fill_slots(block_rows, slot_index, experts, capacity):
    entry_count = slot_index.shape[0]
    source_row = jnp.arange(entry_count, dtype=jnp.int32) // 2
    slot_row = jnp.zeros((experts * capacity + 1,), jnp.int32).at[slot_index].set(source_row)
    filled = jnp.zeros((experts * capacity + 1,), jnp.float32).at[slot_index].set(1.0)
    chosen = block_rows[slot_row[:experts * capacity]]
    return chosen * filled[:experts * capacity, None].astype(block_rows.dtype)


def route_weights(block_ids, group_logits, pair_logits, kept, exp_group):
    group_pick = block_ids[:, 0] // exp_group
    group_exp = jnp.exp(group_logits)
    columns = jnp.arange(group_logits.shape[1], dtype=jnp.int32)
    chosen = jnp.sum(jnp.where(columns[None, :] == group_pick[:, None], group_exp, 0.0), axis=1)
    chosen = chosen / jnp.sum(group_exp, axis=1)
    pair_exp = jnp.exp(pair_logits)
    weights = pair_exp / jnp.sum(pair_exp, axis=1, keepdims=True) * chosen[:, None]
    return weights * kept.reshape(-1, 2).astype(weights.dtype)


def expert_apply(operands):
    slot_rows, gate_matrix, up_matrix, down_matrix = operands
    gate = jnp.dot(slot_rows, gate_matrix, preferred_element_type=jnp.float32)
    up_part = jnp.dot(slot_rows, up_matrix, preferred_element_type=jnp.float32)
    hidden = (jax.nn.silu(gate) * up_part).astype(jnp.bfloat16)
    width = FF // N_TP
    total = jnp.zeros((slot_rows.shape[0], D), jnp.float32)
    for column in range(N_TP):
        term = lax.dot_general(hidden[:, column * width:(column + 1) * width],
                               down_matrix[:, column * width:(column + 1) * width],
                               (((1,), (1,)), ((), ())), preferred_element_type=jnp.float32)
        rounded = lax.optimization_barrier(term.astype(jnp.bfloat16))
        total = total + rounded.astype(jnp.float32)
    return total.astype(jnp.bfloat16)


def combine_block(returned, slot_index, weights):
    limit = returned.shape[0] - 1
    picked = returned[jnp.clip(slot_index, 0, limit)].astype(jnp.float32)
    picked = picked.reshape(weights.shape[0], 2, -1)
    return jnp.sum(picked * weights[:, :, None], axis=1).astype(jnp.bfloat16)


def reference(tokens, norm_gain, gate_weight, up_weight, down_weight, expert_ids, group_logits, pair_logits):
    scaled = norm_gain[None, :, None]
    gate_out = (scaled * gate_weight).astype(jnp.bfloat16)
    up_out = (scaled * up_weight).astype(jnp.bfloat16)
    down_out = down_weight.astype(jnp.bfloat16)
    id_blocks = expert_ids.reshape(N_FS, TOK_DEV, 2)
    token_blocks = tokens.reshape(N_FS, TOK_DEV, D)
    slot_index, kept = jax.vmap(partial(routing, experts=EXPERTS, capacity=CAP))(id_blocks)
    buffers = jax.vmap(partial(fill_slots, experts=EXPERTS, capacity=CAP))(token_blocks, slot_index)
    buffers = buffers.reshape(N_FS, EXPERTS, CAP, D).transpose(1, 0, 2, 3).reshape(EXPERTS, N_FS * CAP, D)
    results = lax.map(expert_apply, (buffers, gate_out, up_out, down_out))
    results = results.reshape(EXPERTS, N_FS, CAP, D).transpose(1, 0, 2, 3).reshape(N_FS, EXPERTS * CAP, D)
    weights = jax.vmap(partial(route_weights, exp_group=EXP_GROUP))(
        id_blocks, group_logits.reshape(N_FS, TOK_DEV, -1), pair_logits.reshape(N_FS, TOK_DEV, 2), kept)
    mixed = jax.vmap(combine_block)(results, slot_index, weights)
    return (mixed.reshape(TOKENS, D), gate_out, up_out, down_out)
```

```python
import functools

import jax
import jax.numpy as jnp
from jax import lax
from jax.experimental import pallas as pl
from jax.experimental.pallas import tpu as pltpu
from jax.sharding import PartitionSpec as P

MESH = pl.DeviceIdType.MESH
BF16 = jnp.bfloat16
F32 = jnp.float32


def each(count, step):
    if count <= 4:
        for i in range(count):
            step(i)
    else:
        lax.fori_loop(0, count, lambda i, c: (step(i), c)[1], 0)


def exchange_kernel(
    n_grp, n_fs, n_tp,
    out_ref, gate_in, up_in, down_in,
    ret, gate_out, up_out, down_out,
    piece, hidden, own, pair_send, pair_recv, x_send, x_recv, result,
    local_sem, slot_s, slot_r, wz_s, wz_r, wy_s, wy_r,
    gx_s, gx_r, gd_s, gd_r, gf_s, gf_r, pr_s, pr_r, xx_s, xx_r, rt_s, rt_r,
):
    g, f, t = lax.axis_index("grp"), lax.axis_index("fs"), lax.axis_index("tp")
    n_x = n_tp // 2
    chip, core = t // 2, lax.rem(t, 2)
    partner = chip * 2 + 1 - core
    width = piece.shape[3]
    block = gate_in.shape[1]
    share = block // n_grp

    def fs_at(k):
        return lax.rem(f + k, n_fs)

    def grp_at(k):
        return lax.rem(g + k, n_grp)

    def chip_at(k):
        return lax.rem(chip + k, n_x)

    def rcopy(src, dst, ssem, rsem, axis, peer):
        return pltpu.make_async_remote_copy(
            src_ref=src, dst_ref=dst, send_sem=ssem, recv_sem=rsem,
            device_id={axis: peer}, device_id_type=MESH,
        )

    barrier = pltpu.get_barrier_semaphore()

    def greet(axis, peer):
        pl.semaphore_signal(barrier, inc=1, device_id={axis: peer}, device_id_type=MESH)

    each(n_fs - 1, lambda i: greet("fs", fs_at(i + 1)))
    each(n_grp - 1, lambda i: greet("grp", grp_at(i + 1)))
    each(n_x - 1, lambda i: greet("tp", chip_at(i + 1) * 2 + core))
    greet("tp", partner)
    pl.semaphore_wait(barrier, n_fs - 1 + n_grp - 1 + n_x - 1 + 1)

    weights = ((gate_in, gate_out), (up_in, up_out), (down_in, down_out))

    def slot_copy(k, source):
        return rcopy(out_ref.at[fs_at(k)], piece.at[t, source], slot_s.at[k],
                     slot_r.at[n_fs - k], "fs", fs_at(k))

    def slot_arrival(k):
        return rcopy(out_ref.at[f], piece.at[t, fs_at(k)], slot_s.at[k], slot_r.at[k], "fs", fs_at(k))

    each(n_fs - 1, lambda i: slot_copy(i + 1, f).start())
    own_slots = pltpu.make_async_copy(out_ref.at[f], piece.at[t, f], local_sem.at[3])
    own_slots.start()

    def w_rows(source, part):
        return pl.ds(source * block + part * share, share)

    def wz_copy(m, k):
        w_in, w_out = weights[m]
        return rcopy(w_in.at[fs_at(k), pl.ds(g * share, share)], w_out.at[w_rows(f, g)],
                     wz_s.at[m, k], wz_r.at[m, n_fs - k], "fs", fs_at(k))

    def wz_arrival(m, k):
        w_in, w_out = weights[m]
        return rcopy(w_in.at[fs_at(k), pl.ds(g * share, share)], w_out.at[w_rows(fs_at(k), g)],
                     wz_s.at[m, k], wz_r.at[m, k], "fs", fs_at(k))

    def wy_copy(m, k, j):
        w_out = weights[m][1]
        rows = w_rows(fs_at(k), g)
        return rcopy(w_out.at[rows], w_out.at[rows], wy_s.at[m, k, j],
                     wy_r.at[m, k, n_grp - j], "grp", grp_at(j))

    def wy_arrival(m, k, j):
        w_out = weights[m][1]
        rows = w_rows(fs_at(k), grp_at(j))
        return rcopy(w_out.at[rows], w_out.at[rows], wy_s.at[m, k, j],
                     wy_r.at[m, k, j], "grp", grp_at(j))

    own_weights = []
    for m in range(3):
        w_in, w_out = weights[m]
        each(n_fs - 1, lambda i: wz_copy(m, i + 1).start())
        copy = pltpu.make_async_copy(w_in.at[f], w_out.at[pl.ds(f * block, block)], local_sem.at[m])
        copy.start()
        own_weights.append(copy)

    def forward(m, k):
        wz_arrival(m, k).wait_recv()
        for j in range(1, n_grp):
            wy_copy(m, k, j).start()

    def gx_copy(k, j):
        src = piece.at[t, fs_at(k)]
        return rcopy(src, src, gx_s.at[k, j], gx_r.at[k, n_x - j], "tp", chip_at(j) * 2 + core)

    def gx_arrival(k, j):
        src = piece.at[chip_at(j) * 2 + core, fs_at(k)]
        return rcopy(src, src, gx_s.at[k, j], gx_r.at[k, j], "tp", chip_at(j) * 2 + core)

    def gd_copy(k):
        src = piece.at[t, fs_at(k)]
        return rcopy(src, src, gd_s.at[k], gd_r.at[k], "tp", partner)

    def gd_arrival(k):
        src = piece.at[partner, fs_at(k)]
        return rcopy(src, src, gd_s.at[k], gd_r.at[k], "tp", partner)

    def gf_copy(k, j):
        src = piece.at[chip_at(j) * 2 + core, fs_at(k)]
        return rcopy(src, src, gf_s.at[k, j], gf_r.at[k, j], "tp", partner)

    def gf_arrival(k, j):
        src = piece.at[chip_at(j) * 2 + 1 - core, fs_at(k)]
        return rcopy(src, src, gf_s.at[k, j], gf_r.at[k, j], "tp", partner)

    def spread(k):
        for j in range(1, n_x):
            gx_copy(k, j).start()
        gd_copy(k).start()

    own_slots.wait()
    spread(0)

    def spread_arrived(i):
        slot_arrival(i + 1).wait_recv()
        spread(i + 1)

    each(n_fs - 1, spread_arrived)

    def hand_over(k):
        for j in range(1, n_x):
            gx_arrival(k, j).wait_recv()
            gf_copy(k, j).start()

    hand_over(0)

    def hand_and_forward(i):
        hand_over(i + 1)
        forward(0, i + 1)

    each(n_fs - 1, hand_and_forward)
    each(n_fs - 1, lambda i: forward(1, i + 1))

    def all_in(m):
        own_weights[m].wait()
        for j in range(1, n_grp):
            each(n_fs - 1, lambda i: wy_arrival(m, i + 1, j).wait_recv())

    all_in(0)
    all_in(1)

    def make_hidden(k):
        source = fs_at(k)
        gd_arrival(k).wait_recv()
        for j in range(1, n_x):
            gf_arrival(k, j).wait_recv()
        gate = up = None
        for p in range(n_tp):
            rows = piece[p, source]
            cols = pl.ds(p * width, width)
            gate_part = jnp.dot(rows, gate_out[cols, :], preferred_element_type=F32)
            up_part = jnp.dot(rows, up_out[cols, :], preferred_element_type=F32)
            gate = gate_part if gate is None else gate + gate_part
            up = up_part if up is None else up + up_part
        hidden[k] = (gate / (1.0 + jnp.exp(-gate)) * up).astype(BF16)

    def hidden_and_forward(i):
        make_hidden(i + 1)
        forward(2, i + 1)

    each(n_fs - 1, hidden_and_forward)
    make_hidden(0)
    all_in(2)

    def term(k, j, to_core):
        column = (chip_at(j) * 2 + to_core) * width
        rows = down_out[pl.ds(pl.multiple_of(column, width), width), :]
        return lax.dot_general(hidden[k], rows, (((1,), (1,)), ((), ())), preferred_element_type=F32)

    def pr_copy(k):
        return rcopy(pair_send.at[k], pair_recv.at[k], pr_s.at[k], pr_r.at[k], "tp", partner)

    def stage_pair(k):
        for j in range(n_x):
            pair_send[k, j] = term(k, j, 1 - core).astype(BF16)
        pr_copy(k).start()
        for j in range(n_x):
            own[k, j] = term(k, j, core)

    def xx_copy(k, j):
        return rcopy(x_send.at[k, j], x_recv.at[k, n_x - j], xx_s.at[k, j], xx_r.at[k, n_x - j],
                     "tp", chip_at(j) * 2 + core)

    def xx_arrival(k, j):
        return rcopy(x_send.at[k, j], x_recv.at[k, j], xx_s.at[k, j], xx_r.at[k, j],
                     "tp", chip_at(j) * 2 + core)

    def stage_chip(k):
        pr_copy(k).wait_recv()
        for j in range(1, n_x):
            x_send[k, j] = (own[k, j] + pair_recv[k, j].astype(F32)).astype(BF16)
            xx_copy(k, j).start()
        own[k, 0] = own[k, 0] + pair_recv[k, 0].astype(F32)

    def rt_copy(k):
        return rcopy(result.at[k], ret.at[f], rt_s.at[k], rt_r.at[n_fs - k], "fs", fs_at(k))

    def rt_arrival(k):
        return rcopy(result.at[k], ret.at[fs_at(k)], rt_s.at[k], rt_r.at[k], "fs", fs_at(k))

    def total(k):
        acc = own[k, 0]
        for j in range(1, n_x):
            xx_arrival(k, j).wait_recv()
            acc = acc + x_recv[k, j].astype(F32)
        return acc.astype(BF16)

    def stage_home(k):
        result[k] = total(k)
        rt_copy(k).start()

    def order(i):
        return i + 1 if n_fs <= 4 and i + 1 < n_fs else lax.rem(i + 1, n_fs)

    stage_pair(order(0))

    def pair_and_chip(i):
        stage_pair(order(i + 1))
        stage_chip(order(i))

    each(n_fs - 1, pair_and_chip)
    stage_chip(order(n_fs - 1))
    each(n_fs - 1, lambda i: stage_home(i + 1))
    ret[f] = total(0)
    each(n_fs - 1, lambda i: rt_arrival(i + 1).wait_recv())

    def drain_peer(i):
        k = i + 1
        slot_copy(k, f).wait_send()
        rt_copy(k).wait_send()
        for m in range(3):
            wz_copy(m, k).wait_send()
            for j in range(1, n_grp):
                wy_copy(m, k, j).wait_send()

    def drain_chunk(k):
        gd_copy(k).wait_send()
        pr_copy(k).wait_send()
        for j in range(1, n_x):
            gx_copy(k, j).wait_send()
            gf_copy(k, j).wait_send()
            xx_copy(k, j).wait_send()

    each(n_fs - 1, drain_peer)
    each(n_fs, drain_chunk)


def exchange(n_grp, n_fs, n_tp, outgoing, gate, up, down):
    n_x = n_tp // 2
    cap, width = outgoing.shape[1:]
    block, hid = gate.shape[1:]
    vmem = pl.BlockSpec(memory_space=pltpu.VMEM)
    dma = pltpu.SemaphoreType.DMA
    matrix = jax.ShapeDtypeStruct((n_fs * block, hid), BF16)
    chunk = (n_fs, n_x, cap, width)
    sem_shapes = [
        (4,), (n_fs,), (n_fs,), (3, n_fs), (3, n_fs), (3, n_fs, n_grp), (3, n_fs, n_grp),
        (n_fs, n_x), (n_fs, n_x), (n_fs,), (n_fs,), (n_fs, n_x), (n_fs, n_x),
        (n_fs,), (n_fs,), (n_fs, n_x), (n_fs, n_x), (n_fs,), (n_fs,),
    ]
    return pl.pallas_call(
        functools.partial(exchange_kernel, n_grp, n_fs, n_tp),
        out_shape=(jax.ShapeDtypeStruct((n_fs, cap, width), BF16), matrix, matrix, matrix),
        in_specs=[vmem] * 4,
        out_specs=(vmem,) * 4,
        scratch_shapes=[
            pltpu.VMEM((n_tp, n_fs, cap, width), BF16),
            pltpu.VMEM((n_fs, cap, hid), BF16),
            pltpu.VMEM(chunk, F32),
            pltpu.VMEM(chunk, BF16),
            pltpu.VMEM(chunk, BF16),
            pltpu.VMEM(chunk, BF16),
            pltpu.VMEM(chunk, BF16),
            pltpu.VMEM((n_fs, cap, width), BF16),
        ] + [dma(s) for s in sem_shapes],
        compiler_params=pltpu.CompilerParams(
            collective_id=0, has_side_effects=True, vmem_limit_bytes=56 * 1024 * 1024
        ),
    )(outgoing, gate, up, down)


def body(
    tokens, norm_gain, gate_weight, up_weight, down_weight, expert_ids, group_logits, pair_logits
):
    n_grp, n_fs, n_tp = (lax.axis_size(a) for a in ("grp", "fs", "tp"))
    experts = gate_weight.shape[0]
    tok_rows = tokens.shape[0]
    capacity = 5 * tok_rows * 2 // (4 * experts)
    padded = -(-capacity // 16) * 16
    slots = experts * padded

    columns = jnp.arange(experts, dtype=jnp.int32)
    named = [(expert_ids[:, k, None] == columns[None, :]).astype(F32) for k in range(2)]
    rows = jnp.arange(tok_rows, dtype=jnp.int32)
    earlier = (rows[None, :] < rows[:, None]).astype(BF16)
    before = jnp.dot(earlier, (named[0] + named[1]).astype(BF16), preferred_element_type=F32)
    picks, kept = [], []
    for k in range(2):
        rank = jnp.sum(before * named[k], axis=1).astype(jnp.int32)
        kept.append(rank < capacity)
        picks.append(jnp.where(kept[k], expert_ids[:, k] * padded + rank, slots))
    slot_ids = jnp.arange(slots, dtype=jnp.int32)
    place = [(picks[k][:, None] == slot_ids[None, :]).astype(BF16) for k in range(2)]
    outgoing = lax.dot_general(
        place[0] + place[1], tokens, (((0,), (0,)), ((), ())), preferred_element_type=F32
    ).astype(BF16).reshape(experts, padded, -1)

    scaled = norm_gain[None, :, None]
    gate_cast = (scaled * gate_weight).astype(BF16)
    up_cast = (scaled * up_weight).astype(BF16)
    down_cast = down_weight.astype(BF16)
    returned, gate_here, up_here, down_here = exchange(
        n_grp, n_fs, n_tp, outgoing, gate_cast, up_cast, down_cast
    )
    returned = returned.reshape(slots, -1)

    group_exp = jnp.exp(group_logits)
    group_count = group_logits.shape[1]
    group_pick = expert_ids[:, 0] // (experts // group_count)
    groups = jnp.arange(group_count, dtype=jnp.int32)
    chosen = jnp.sum(jnp.where(groups[None, :] == group_pick[:, None], group_exp, 0.0), axis=1)
    chosen = chosen / jnp.sum(group_exp, axis=1)
    pair_exp = jnp.exp(pair_logits)
    weights = pair_exp / jnp.sum(pair_exp, axis=1, keepdims=True) * chosen[:, None]
    mixed = 0.0
    for k in range(2):
        weight = weights[:, k] * kept[k].astype(F32)
        picked = jnp.dot(place[k], returned, preferred_element_type=F32)
        mixed = mixed + picked * weight[:, None]
    return (mixed.astype(BF16), gate_here[None], up_here[None], down_here[None])


def solution(mesh):
    placed = (
        P(("grp", "fs"), "tp"),
        P("fs"),
        P(None, "fs", "tp"),
        P(None, "fs", "tp"),
        P(None, "fs", "tp"),
        P(("grp", "fs"), None),
        P(("grp", "fs"), None),
        P(("grp", "fs"), None),
    )
    return jax.shard_map(
        body,
        mesh=mesh,
        in_specs=placed,
        out_specs=(
            P(("grp", "fs"), "tp"),
            P(("grp", "fs"), None, "tp"),
            P(("grp", "fs"), None, "tp"),
            P(("grp", "fs"), None, "tp"),
        ),
        check_vma=False,
    )
```

```python
import functools

import jax
import jax.numpy as jnp
from jax import lax
from jax.experimental import pallas as pl
from jax.experimental.pallas import tpu as pltpu
from jax.sharding import PartitionSpec as P

MESH = pl.DeviceIdType.MESH
BF16 = jnp.bfloat16
F32 = jnp.float32


def each(count, step):
    if count <= 4:
        for i in range(count):
            step(i)
    else:
        lax.fori_loop(0, count, lambda i, c: (step(i), c)[1], 0)


def exchange_kernel(
    n_grp, n_fs, n_tp, capacity,
    tokens, gain, id_rows, id_cols, group_logits, pair_logits, gate_in, up_in, down_in,
    mixed, gate_out, up_out, down_out,
    out_ref, raw, cast, ret, mix, piece, hidden, own, pair_send, pair_recv, x_send, x_recv, result,
    local_sem, raw_sem, slot_s, slot_r, wz_s, wz_r, wy_s, wy_r,
    gx_s, gx_r, gd_s, gd_r, gf_s, gf_r, pr_s, pr_r, xx_s, xx_r, rt_s, rt_r,
):
    g, f, t = lax.axis_index("grp"), lax.axis_index("fs"), lax.axis_index("tp")
    n_x = n_tp // 2
    chip, core = t // 2, lax.rem(t, 2)
    partner = chip * 2 + 1 - core
    width = piece.shape[3]
    block = cast.shape[2]
    tok_rows, padded = tokens.shape[0], out_ref.shape[1]
    experts = n_fs
    share = block // n_grp

    def fs_at(k):
        return lax.rem(f + k, n_fs)

    def grp_at(k):
        return lax.rem(g + k, n_grp)

    def chip_at(k):
        return lax.rem(chip + k, n_x)

    def rcopy(src, dst, ssem, rsem, axis, peer):
        return pltpu.make_async_remote_copy(
            src_ref=src, dst_ref=dst, send_sem=ssem, recv_sem=rsem,
            device_id={axis: peer}, device_id_type=MESH,
        )

    raw_copies = [
        pltpu.make_async_copy(w, raw.at[m], raw_sem.at[m])
        for m, w in enumerate((gate_in, up_in, down_in))
    ]
    for copy in raw_copies:
        copy.start()

    barrier = pltpu.get_barrier_semaphore()

    def greet(axis, peer):
        pl.semaphore_signal(barrier, inc=1, device_id={axis: peer}, device_id_type=MESH)

    each(n_fs - 1, lambda i: greet("fs", fs_at(i + 1)))
    each(n_grp - 1, lambda i: greet("grp", grp_at(i + 1)))
    each(n_x - 1, lambda i: greet("tp", chip_at(i + 1) * 2 + core))
    greet("tp", partner)

    def ints(shape, axis):
        return lax.broadcasted_iota(jnp.int32, shape, axis)

    def route(ids, axis):
        shape = (experts, tok_rows) if axis == 0 else (tok_rows, experts)
        named = [(ints(shape, axis) == i).astype(F32) for i in ids]
        square = (tok_rows, tok_rows)
        earlier = (ints(square, axis) < ints(square, 1 - axis)).astype(F32).astype(BF16)
        both = (named[0] + named[1]).astype(BF16)
        pair = (both, earlier) if axis == 0 else (earlier, both)
        before = jnp.dot(*pair, preferred_element_type=F32)
        picks, kept = [], []
        for i, name in zip(ids, named):
            rank = jnp.sum(before * name, axis=axis, keepdims=True)
            kept.append(rank < capacity)
            slot = i * padded + rank.astype(jnp.int32)
            picks.append(jnp.where(rank < capacity, slot, -1))
        return picks, kept

    row_picks, _ = route([id_rows[0:1, :], id_rows[1:2, :]], 0)

    def fill(k):
        e = fs_at(k)
        slot = ints((padded, tok_rows), 0) + e * padded
        named = (slot == row_picks[0]) | (slot == row_picks[1])
        place = jnp.where(named, 1.0, 0.0).astype(BF16)
        out_ref[e] = jnp.dot(place, tokens[...], preferred_element_type=F32).astype(BF16)

    each(n_fs - 1, lambda i: fill(i + 1))
    pl.semaphore_wait(barrier, n_fs - 1 + n_grp - 1 + n_x - 1 + 1)

    weights = (
        (cast.at[0], gate_out), (cast.at[1], up_out), (cast.at[2], down_out)
    )

    def slot_copy(k, source):
        return rcopy(out_ref.at[fs_at(k)], piece.at[t, source], slot_s.at[k],
                     slot_r.at[n_fs - k], "fs", fs_at(k))

    def slot_arrival(k):
        return rcopy(out_ref.at[f], piece.at[t, fs_at(k)], slot_s.at[k], slot_r.at[k], "fs", fs_at(k))

    each(n_fs - 1, lambda i: slot_copy(i + 1, f).start())
    fill(0)
    own_slots = pltpu.make_async_copy(out_ref.at[f], piece.at[t, f], local_sem.at[3])
    own_slots.start()

    def w_rows(source, part):
        return pl.ds(source * block + part * share, share)

    def wz_copy(m, k):
        w_in, w_out = weights[m]
        return rcopy(w_in.at[fs_at(k), pl.ds(g * share, share)], w_out.at[w_rows(f, g)],
                     wz_s.at[m, k], wz_r.at[m, n_fs - k], "fs", fs_at(k))

    def wz_arrival(m, k):
        w_in, w_out = weights[m]
        return rcopy(w_in.at[fs_at(k), pl.ds(g * share, share)], w_out.at[w_rows(fs_at(k), g)],
                     wz_s.at[m, k], wz_r.at[m, k], "fs", fs_at(k))

    def wy_copy(m, k, j):
        w_out = weights[m][1]
        rows = w_rows(fs_at(k), g)
        return rcopy(w_out.at[rows], w_out.at[rows], wy_s.at[m, k, j],
                     wy_r.at[m, k, n_grp - j], "grp", grp_at(j))

    def wy_arrival(m, k, j):
        w_out = weights[m][1]
        rows = w_rows(fs_at(k), grp_at(j))
        return rcopy(w_out.at[rows], w_out.at[rows], wy_s.at[m, k, j],
                     wy_r.at[m, k, j], "grp", grp_at(j))

    own_weights = []
    for m in range(3):
        w_in, w_out = weights[m]
        raw_copies[m].wait()

        def round_block(e):
            if m < 2:
                cast[m, e] = (gain[...] * raw[m, e]).astype(BF16)
            else:
                cast[m, e] = raw[m, e].astype(BF16)

        each(n_fs, round_block)
        each(n_fs - 1, lambda i: wz_copy(m, i + 1).start())
        copy = pltpu.make_async_copy(w_in.at[f], w_out.at[pl.ds(f * block, block)], local_sem.at[m])
        copy.start()
        own_weights.append(copy)

    def forward(m, k):
        wz_arrival(m, k).wait_recv()
        for j in range(1, n_grp):
            wy_copy(m, k, j).start()

    def gx_copy(k, j):
        src = piece.at[t, fs_at(k)]
        return rcopy(src, src, gx_s.at[k, j], gx_r.at[k, n_x - j], "tp", chip_at(j) * 2 + core)

    def gx_arrival(k, j):
        src = piece.at[chip_at(j) * 2 + core, fs_at(k)]
        return rcopy(src, src, gx_s.at[k, j], gx_r.at[k, j], "tp", chip_at(j) * 2 + core)

    def gd_copy(k):
        src = piece.at[t, fs_at(k)]
        return rcopy(src, src, gd_s.at[k], gd_r.at[k], "tp", partner)

    def gd_arrival(k):
        src = piece.at[partner, fs_at(k)]
        return rcopy(src, src, gd_s.at[k], gd_r.at[k], "tp", partner)

    def gf_copy(k, j):
        src = piece.at[chip_at(j) * 2 + core, fs_at(k)]
        return rcopy(src, src, gf_s.at[k, j], gf_r.at[k, j], "tp", partner)

    def gf_arrival(k, j):
        src = piece.at[chip_at(j) * 2 + 1 - core, fs_at(k)]
        return rcopy(src, src, gf_s.at[k, j], gf_r.at[k, j], "tp", partner)

    def spread(k):
        for j in range(1, n_x):
            gx_copy(k, j).start()
        gd_copy(k).start()

    own_slots.wait()
    spread(0)

    ids = [id_cols[:, k : k + 1] for k in range(2)]
    picks, kept = route(ids, 1)
    group_exp = jnp.exp(group_logits[...])
    group_count = group_exp.shape[1]
    low = ints(group_exp.shape, 1) * (experts // group_count)
    member = (ids[0] >= low) & (ids[0] < low + experts // group_count)
    chosen = jnp.sum(jnp.where(member, group_exp, 0.0), axis=1, keepdims=True)
    chosen = chosen / jnp.sum(group_exp, axis=1, keepdims=True)
    pair_exp = jnp.exp(pair_logits[...])
    pair_weight = pair_exp / jnp.sum(pair_exp, axis=1, keepdims=True) * chosen
    mix_weights = [
        jnp.where(kept[k], pair_weight[:, k : k + 1], 0.0) for k in range(2)
    ]

    def blend(k):
        e = fs_at(k)
        slot = ints((tok_rows, padded), 1) + e * padded
        named = (slot == picks[0]) | (slot == picks[1])
        place = jnp.where(named, 1.0, 0.0).astype(BF16)
        weight = jnp.where(ids[0] == e, mix_weights[0], 0.0)
        weight = weight + jnp.where(ids[1] == e, mix_weights[1], 0.0)
        return jnp.dot(place, ret[e], preferred_element_type=F32) * weight

    def spread_arrived(i):
        slot_arrival(i + 1).wait_recv()
        spread(i + 1)

    each(n_fs - 1, spread_arrived)

    def hand_over(k):
        for j in range(1, n_x):
            gx_arrival(k, j).wait_recv()
            gf_copy(k, j).start()

    hand_over(0)

    def hand_and_forward(i):
        hand_over(i + 1)
        forward(0, i + 1)

    each(n_fs - 1, hand_and_forward)
    each(n_fs - 1, lambda i: forward(1, i + 1))

    def all_in(m):
        own_weights[m].wait()
        for j in range(1, n_grp):
            each(n_fs - 1, lambda i: wy_arrival(m, i + 1, j).wait_recv())

    all_in(0)
    all_in(1)

    def make_hidden(k):
        source = fs_at(k)
        gd_arrival(k).wait_recv()
        for j in range(1, n_x):
            gf_arrival(k, j).wait_recv()
        gate = up = None
        for p in range(n_tp):
            rows = piece[p, source]
            cols = pl.ds(p * width, width)
            gate_part = jnp.dot(rows, gate_out[cols, :], preferred_element_type=F32)
            up_part = jnp.dot(rows, up_out[cols, :], preferred_element_type=F32)
            gate = gate_part if gate is None else gate + gate_part
            up = up_part if up is None else up + up_part
        hidden[k] = (gate / (1.0 + jnp.exp(-gate)) * up).astype(BF16)

    def hidden_and_forward(i):
        make_hidden(i + 1)
        forward(2, i + 1)

    each(n_fs - 1, hidden_and_forward)
    make_hidden(0)
    all_in(2)

    def term(k, j, to_core):
        column = (chip_at(j) * 2 + to_core) * width
        rows = down_out[pl.ds(pl.multiple_of(column, width), width), :]
        return lax.dot_general(hidden[k], rows, (((1,), (1,)), ((), ())), preferred_element_type=F32)

    def pr_copy(k):
        return rcopy(pair_send.at[k], pair_recv.at[k], pr_s.at[k], pr_r.at[k], "tp", partner)

    def stage_pair(k):
        for j in range(n_x):
            pair_send[k, j] = term(k, j, 1 - core).astype(BF16)
        pr_copy(k).start()
        for j in range(n_x):
            own[k, j] = term(k, j, core)

    def xx_copy(k, j):
        return rcopy(x_send.at[k, j], x_recv.at[k, n_x - j], xx_s.at[k, j], xx_r.at[k, n_x - j],
                     "tp", chip_at(j) * 2 + core)

    def xx_arrival(k, j):
        return rcopy(x_send.at[k, j], x_recv.at[k, j], xx_s.at[k, j], xx_r.at[k, j],
                     "tp", chip_at(j) * 2 + core)

    def stage_chip(k):
        pr_copy(k).wait_recv()
        for j in range(1, n_x):
            x_send[k, j] = (own[k, j] + pair_recv[k, j].astype(F32)).astype(BF16)
            xx_copy(k, j).start()
        own[k, 0] = own[k, 0] + pair_recv[k, 0].astype(F32)

    def rt_copy(k):
        return rcopy(result.at[k], ret.at[f], rt_s.at[k], rt_r.at[n_fs - k], "fs", fs_at(k))

    def rt_arrival(k):
        return rcopy(result.at[k], ret.at[fs_at(k)], rt_s.at[k], rt_r.at[k], "fs", fs_at(k))

    def total(k):
        acc = own[k, 0]
        for j in range(1, n_x):
            xx_arrival(k, j).wait_recv()
            acc = acc + x_recv[k, j].astype(F32)
        return acc.astype(BF16)

    def stage_home(k):
        result[k] = total(k)
        rt_copy(k).start()

    def order(i):
        return (2, 1, 3, 0)[i] if n_fs == 4 else lax.rem(i + 1, n_fs)

    stage_pair(order(0))

    def pair_and_chip(i):
        stage_pair(order(i + 1))
        stage_chip(order(i))

    each(n_fs - 1, pair_and_chip)
    stage_chip(order(n_fs - 1))
    each(n_fs - 1, lambda i: stage_home(order(i)))
    ret[f] = total(0)
    mix[...] = blend(0)

    def collect(i):
        k = order(i) if n_fs != 4 else (2, 3, 1)[i]
        rt_arrival(k).wait_recv()
        mix[...] += blend(k)

    each(n_fs - 1, collect)
    mixed[...] = mix[...].astype(BF16)

    def drain_peer(i):
        k = i + 1
        slot_copy(k, f).wait_send()
        rt_copy(k).wait_send()
        for m in range(3):
            wz_copy(m, k).wait_send()
            for j in range(1, n_grp):
                wy_copy(m, k, j).wait_send()

    def drain_chunk(k):
        gd_copy(k).wait_send()
        pr_copy(k).wait_send()
        for j in range(1, n_x):
            gx_copy(k, j).wait_send()
            gf_copy(k, j).wait_send()
            xx_copy(k, j).wait_send()

    each(n_fs - 1, drain_peer)
    each(n_fs, drain_chunk)


def body(
    tokens, norm_gain, gate_weight, up_weight, down_weight, expert_ids, group_logits, pair_logits
):
    n_grp, n_fs, n_tp = (lax.axis_size(a) for a in ("grp", "fs", "tp"))
    n_x = n_tp // 2
    experts, block, hid = gate_weight.shape
    tok_rows, width = tokens.shape
    capacity = 5 * tok_rows * 2 // (4 * experts)
    cap = -(-capacity // 16) * 16
    vmem = pl.BlockSpec(memory_space=pltpu.VMEM)
    hbm = pl.BlockSpec(memory_space=pl.ANY)
    dma = pltpu.SemaphoreType.DMA
    matrix = jax.ShapeDtypeStruct((n_fs * block, hid), BF16)
    chunk = (n_fs, n_x, cap, width)
    sem_shapes = [
        (4,), (3,), (n_fs,), (n_fs,), (3, n_fs), (3, n_fs), (3, n_fs, n_grp), (3, n_fs, n_grp),
        (n_fs, n_x), (n_fs, n_x), (n_fs,), (n_fs,), (n_fs, n_x), (n_fs, n_x),
        (n_fs,), (n_fs,), (n_fs, n_x), (n_fs, n_x), (n_fs,), (n_fs,),
    ]
    mixed, *matrices = pl.pallas_call(
        functools.partial(exchange_kernel, n_grp, n_fs, n_tp, capacity),
        out_shape=(jax.ShapeDtypeStruct((tok_rows, width), BF16), matrix, matrix, matrix),
        in_specs=[vmem] * 6 + [hbm] * 3,
        out_specs=(vmem,) * 4,
        scratch_shapes=[
            pltpu.VMEM((n_fs, cap, width), BF16),
            pltpu.VMEM((3, n_fs, block, hid), F32),
            pltpu.VMEM((3, n_fs, block, hid), BF16),
            pltpu.VMEM((n_fs, cap, width), BF16),
            pltpu.VMEM((tok_rows, width), F32),
            pltpu.VMEM((n_tp, n_fs, cap, width), BF16),
            pltpu.VMEM((n_fs, cap, hid), BF16),
            pltpu.VMEM(chunk, F32),
            pltpu.VMEM(chunk, BF16),
            pltpu.VMEM(chunk, BF16),
            pltpu.VMEM(chunk, BF16),
            pltpu.VMEM(chunk, BF16),
            pltpu.VMEM((n_fs, cap, width), BF16),
        ] + [dma(s) for s in sem_shapes],
        compiler_params=pltpu.CompilerParams(
            collective_id=0, has_side_effects=True, vmem_limit_bytes=48 * 1024 * 1024
        ),
    )(
        tokens, norm_gain[:, None], expert_ids.T, expert_ids, group_logits, pair_logits,
        gate_weight, up_weight, down_weight,
    )
    return (mixed, *(m[None] for m in matrices))


def solution(mesh):
    placed = (
        P(("grp", "fs"), "tp"),
        P("fs"),
        P(None, "fs", "tp"),
        P(None, "fs", "tp"),
        P(None, "fs", "tp"),
        P(("grp", "fs"), None),
        P(("grp", "fs"), None),
        P(("grp", "fs"), None),
    )
    return jax.shard_map(
        body,
        mesh=mesh,
        in_specs=placed,
        out_specs=(
            P(("grp", "fs"), "tp"),
            P(("grp", "fs"), None, "tp"),
            P(("grp", "fs"), None, "tp"),
            P(("grp", "fs"), None, "tp"),
        ),
        check_vma=False,
    )
```

```python
import functools

import jax
import jax.numpy as jnp
from jax import lax
from jax.experimental import pallas as pl
from jax.experimental.pallas import tpu as pltpu
from jax.sharding import PartitionSpec as P

MESH = pl.DeviceIdType.MESH
BF16 = jnp.bfloat16
F32 = jnp.float32


def each(count, step):
    if count <= 4:
        for i in range(count):
            step(i)
    else:
        lax.fori_loop(0, count, lambda i, c: (step(i), c)[1], 0)


def exchange_kernel(
    n_grp, n_fs, n_tp, capacity,
    tokens, gain, id_rows, group_logits, pair_logits, gate_in, up_in, down_in,
    mixed, gate_out, up_out, down_out,
    out_ref, raw, cast, ret, mix, piece, hidden, own, pair_send, pair_recv, x_send, x_recv, result,
    local_sem, raw_sem, slot_s, slot_r, wz_s, wz_r, wy_s, wy_r,
    gx_s, gx_r, gd_s, gd_r, gf_s, gf_r, pr_s, pr_r, xx_s, xx_r, rt_s, rt_r,
):
    g, f, t = lax.axis_index("grp"), lax.axis_index("fs"), lax.axis_index("tp")
    n_x = n_tp // 2
    chip, core = t // 2, lax.rem(t, 2)
    partner = chip * 2 + 1 - core
    width = piece.shape[3]
    block = cast.shape[2]
    tok_rows, padded = tokens.shape[0], out_ref.shape[1]
    experts = n_fs
    share = block // n_grp

    def fs_at(k):
        return lax.rem(f + k, n_fs)

    def outward(i):
        return jnp.where(f < n_fs // 2, i + 1, n_fs - 1 - i)

    def nearest(i):
        if n_fs != 4:
            return outward(i)
        first = jnp.where(f % 2 == 0, 1, 3)
        last = jnp.where(f == 0, 3, jnp.where(f == 3, 1, 2))
        return (first, 6 - first - last, last)[i]

    def grp_at(k):
        return lax.rem(g + k, n_grp)

    def chip_at(k):
        return lax.rem(chip + k, n_x)

    def rcopy(src, dst, ssem, rsem, axis, peer):
        return pltpu.make_async_remote_copy(
            src_ref=src, dst_ref=dst, send_sem=ssem, recv_sem=rsem,
            device_id={axis: peer}, device_id_type=MESH,
        )

    raw_copies = [
        pltpu.make_async_copy(w, raw.at[m], raw_sem.at[m])
        for m, w in enumerate((gate_in, up_in, down_in))
    ]
    for copy in raw_copies:
        copy.start()

    barrier = pltpu.get_barrier_semaphore()

    def greet(axis, peer):
        pl.semaphore_signal(barrier, inc=1, device_id={axis: peer}, device_id_type=MESH)

    each(n_fs - 1, lambda i: greet("fs", fs_at(i + 1)))
    each(n_grp - 1, lambda i: greet("grp", grp_at(i + 1)))
    each(n_x - 1, lambda i: greet("tp", chip_at(i + 1) * 2 + core))
    greet("tp", partner)

    def ints(shape, axis):
        return lax.broadcasted_iota(jnp.int32, shape, axis)

    def route(ids, axis):
        shape = (experts, tok_rows) if axis == 0 else (tok_rows, experts)
        named = [(ints(shape, axis) == i).astype(F32) for i in ids]
        square = (tok_rows, tok_rows)
        earlier = (ints(square, axis) < ints(square, 1 - axis)).astype(F32).astype(BF16)
        both = (named[0] + named[1]).astype(BF16)
        pair = (both, earlier) if axis == 0 else (earlier, both)
        before = jnp.dot(*pair, preferred_element_type=F32)
        picks, kept = [], []
        for i, name in zip(ids, named):
            rank = jnp.sum(before * name, axis=axis, keepdims=True)
            kept.append(rank < capacity)
            slot = i * padded + rank.astype(jnp.int32)
            picks.append(jnp.where(rank < capacity, slot, -1))
        return picks, kept

    row_picks, _ = route([id_rows[0:1, :], id_rows[1:2, :]], 0)

    def fill(k):
        e = fs_at(k)
        slot = ints((padded, tok_rows), 0) + e * padded
        named = (slot == row_picks[0]) | (slot == row_picks[1])
        place = jnp.where(named, 1.0, 0.0).astype(BF16)
        out_ref[e] = jnp.dot(place, tokens[...], preferred_element_type=F32).astype(BF16)

    each(n_fs - 1, lambda i: fill(i + 1))
    pl.semaphore_wait(barrier, n_fs - 1 + n_grp - 1 + n_x - 1 + 1)

    weights = (
        (cast.at[0], gate_out), (cast.at[1], up_out), (cast.at[2], down_out)
    )

    def slot_copy(k, source):
        return rcopy(out_ref.at[fs_at(k)], piece.at[t, source], slot_s.at[k],
                     slot_r.at[n_fs - k], "fs", fs_at(k))

    def slot_arrival(k):
        return rcopy(out_ref.at[f], piece.at[t, fs_at(k)], slot_s.at[k], slot_r.at[k], "fs", fs_at(k))

    each(n_fs - 1, lambda i: slot_copy(outward(i), f).start())
    fill(0)
    own_slots = pltpu.make_async_copy(out_ref.at[f], piece.at[t, f], local_sem.at[3])
    own_slots.start()

    def w_rows(source, part):
        return pl.ds(source * block + part * share, share)

    def wz_copy(m, k):
        w_in, w_out = weights[m]
        return rcopy(w_in.at[fs_at(k), pl.ds(g * share, share)], w_out.at[w_rows(f, g)],
                     wz_s.at[m, k], wz_r.at[m, n_fs - k], "fs", fs_at(k))

    def wz_arrival(m, k):
        w_in, w_out = weights[m]
        return rcopy(w_in.at[fs_at(k), pl.ds(g * share, share)], w_out.at[w_rows(fs_at(k), g)],
                     wz_s.at[m, k], wz_r.at[m, k], "fs", fs_at(k))

    def wy_copy(m, k, j):
        w_out = weights[m][1]
        rows = w_rows(fs_at(k), g)
        return rcopy(w_out.at[rows], w_out.at[rows], wy_s.at[m, k, j],
                     wy_r.at[m, k, n_grp - j], "grp", grp_at(j))

    def wy_arrival(m, k, j):
        w_out = weights[m][1]
        rows = w_rows(fs_at(k), grp_at(j))
        return rcopy(w_out.at[rows], w_out.at[rows], wy_s.at[m, k, j],
                     wy_r.at[m, k, j], "grp", grp_at(j))

    own_weights = []
    for m in range(3):
        w_in, w_out = weights[m]
        raw_copies[m].wait()

        def round_block(e):
            if m < 2:
                cast[m, e] = (gain[...] * raw[m, e]).astype(BF16)
            else:
                cast[m, e] = raw[m, e].astype(BF16)

        each(n_fs, round_block)
        copy = pltpu.make_async_copy(w_in.at[f], w_out.at[pl.ds(f * block, block)], local_sem.at[m])
        copy.start()
        own_weights.append(copy)

    for m in range(3):
        each(n_fs - 1, lambda i: wz_copy(m, outward(i)).start())

    def forward(m, k):
        wz_arrival(m, k).wait_recv()
        for j in range(1, n_grp):
            wy_copy(m, k, j).start()

    def gx_copy(k, j):
        src = piece.at[t, fs_at(k)]
        return rcopy(src, src, gx_s.at[k, j], gx_r.at[k, n_x - j], "tp", chip_at(j) * 2 + core)

    def gx_arrival(k, j):
        src = piece.at[chip_at(j) * 2 + core, fs_at(k)]
        return rcopy(src, src, gx_s.at[k, j], gx_r.at[k, j], "tp", chip_at(j) * 2 + core)

    def gd_copy(k):
        src = piece.at[t, fs_at(k)]
        return rcopy(src, src, gd_s.at[k], gd_r.at[k], "tp", partner)

    def gd_arrival(k):
        src = piece.at[partner, fs_at(k)]
        return rcopy(src, src, gd_s.at[k], gd_r.at[k], "tp", partner)

    def gf_copy(k, j):
        src = piece.at[chip_at(j) * 2 + core, fs_at(k)]
        return rcopy(src, src, gf_s.at[k, j], gf_r.at[k, j], "tp", partner)

    def gf_arrival(k, j):
        src = piece.at[chip_at(j) * 2 + 1 - core, fs_at(k)]
        return rcopy(src, src, gf_s.at[k, j], gf_r.at[k, j], "tp", partner)

    def spread(k):
        for j in range(1, n_x):
            gx_copy(k, j).start()
        gd_copy(k).start()

    own_slots.wait()
    spread(0)

    id_cols = jnp.transpose(id_rows[...])
    ids = [id_cols[:, k : k + 1] for k in range(2)]
    picks, kept = route(ids, 1)
    group_exp = jnp.exp(jnp.transpose(group_logits[...]))
    group_count = group_exp.shape[1]
    low = ints(group_exp.shape, 1) * (experts // group_count)
    member = (ids[0] >= low) & (ids[0] < low + experts // group_count)
    chosen = jnp.sum(jnp.where(member, group_exp, 0.0), axis=1, keepdims=True)
    chosen = chosen / jnp.sum(group_exp, axis=1, keepdims=True)
    pair_exp = jnp.exp(jnp.transpose(pair_logits[...]))
    pair_weight = pair_exp / jnp.sum(pair_exp, axis=1, keepdims=True) * chosen
    mix_weights = [
        jnp.where(kept[k], pair_weight[:, k : k + 1], 0.0) for k in range(2)
    ]

    def blend(k):
        e = fs_at(k)
        slot = ints((tok_rows, padded), 1) + e * padded
        named = (slot == picks[0]) | (slot == picks[1])
        place = jnp.where(named, 1.0, 0.0).astype(BF16)
        weight = jnp.where(ids[0] == e, mix_weights[0], 0.0)
        weight = weight + jnp.where(ids[1] == e, mix_weights[1], 0.0)
        return jnp.dot(place, ret[e], preferred_element_type=F32) * weight

    def spread_arrived(i):
        slot_arrival(nearest(i)).wait_recv()
        spread(nearest(i))

    each(n_fs - 1, spread_arrived)

    def hand_over(k):
        for j in range(1, n_x):
            gx_arrival(k, j).wait_recv()
            gf_copy(k, j).start()

    hand_over(0)

    each(n_fs - 1, lambda i: hand_over(nearest(i)))

    for m in range(3):
        each(n_fs - 1, lambda i: forward(m, nearest(i)))

    def all_in(m):
        own_weights[m].wait()
        for j in range(1, n_grp):
            each(n_fs - 1, lambda i: wy_arrival(m, i + 1, j).wait_recv())

    all_in(0)
    all_in(1)

    def make_hidden(k):
        source = fs_at(k)
        gd_arrival(k).wait_recv()
        for j in range(1, n_x):
            gf_arrival(k, j).wait_recv()
        gate = up = None
        for p in range(n_tp):
            rows = piece[p, source]
            cols = pl.ds(p * width, width)
            gate_part = jnp.dot(rows, gate_out[cols, :], preferred_element_type=F32)
            up_part = jnp.dot(rows, up_out[cols, :], preferred_element_type=F32)
            gate = gate_part if gate is None else gate + gate_part
            up = up_part if up is None else up + up_part
        hidden[k] = (gate / (1.0 + jnp.exp(-gate)) * up).astype(BF16)

    each(n_fs, lambda i: make_hidden(i))
    all_in(2)

    def term(k, j, to_core):
        column = (chip_at(j) * 2 + to_core) * width
        rows = down_out[pl.ds(pl.multiple_of(column, width), width), :]
        return lax.dot_general(hidden[k], rows, (((1,), (1,)), ((), ())), preferred_element_type=F32)

    def pr_copy(k):
        return rcopy(pair_send.at[k], pair_recv.at[k], pr_s.at[k], pr_r.at[k], "tp", partner)

    def stage_pair(k):
        for j in range(n_x):
            pair_send[k, j] = term(k, j, 1 - core).astype(BF16)
        pr_copy(k).start()
        for j in range(n_x):
            own[k, j] = term(k, j, core)

    def xx_copy(k, j):
        return rcopy(x_send.at[k, j], x_recv.at[k, n_x - j], xx_s.at[k, j], xx_r.at[k, n_x - j],
                     "tp", chip_at(j) * 2 + core)

    def xx_arrival(k, j):
        return rcopy(x_send.at[k, j], x_recv.at[k, j], xx_s.at[k, j], xx_r.at[k, j],
                     "tp", chip_at(j) * 2 + core)

    def stage_chip(k):
        pr_copy(k).wait_recv()
        for j in range(1, n_x):
            x_send[k, j] = (own[k, j] + pair_recv[k, j].astype(F32)).astype(BF16)
            xx_copy(k, j).start()
        own[k, 0] = own[k, 0] + pair_recv[k, 0].astype(F32)

    def rt_copy(k):
        return rcopy(result.at[k], ret.at[f], rt_s.at[k], rt_r.at[n_fs - k], "fs", fs_at(k))

    def rt_arrival(k):
        return rcopy(result.at[k], ret.at[fs_at(k)], rt_s.at[k], rt_r.at[k], "fs", fs_at(k))

    def total(k):
        acc = own[k, 0]
        for j in range(1, n_x):
            xx_arrival(k, j).wait_recv()
            acc = acc + x_recv[k, j].astype(F32)
        return acc.astype(BF16)

    def stage_home(k):
        result[k] = total(k)
        rt_copy(k).start()

    def order(i):
        return lax.rem(outward(i) + n_fs, n_fs)

    stage_pair(order(0))

    def pair_and_chip(i):
        stage_pair(order(i + 1))
        stage_chip(order(i))

    each(n_fs - 1, pair_and_chip)
    stage_chip(order(n_fs - 1))
    each(n_fs - 1, lambda i: stage_home(order(i)))
    ret[f] = total(0)
    mix[...] = blend(0)

    def collect(i):
        k = nearest(i)
        rt_arrival(k).wait_recv()
        mix[...] += blend(k)

    each(n_fs - 1, collect)
    mixed[...] = mix[...].astype(BF16)

    def drain_peer(i):
        k = i + 1
        slot_copy(k, f).wait_send()
        rt_copy(k).wait_send()
        for m in range(3):
            wz_copy(m, k).wait_send()
            for j in range(1, n_grp):
                wy_copy(m, k, j).wait_send()

    def drain_chunk(k):
        gd_copy(k).wait_send()
        pr_copy(k).wait_send()
        for j in range(1, n_x):
            gx_copy(k, j).wait_send()
            gf_copy(k, j).wait_send()
            xx_copy(k, j).wait_send()

    each(n_fs - 1, drain_peer)
    each(n_fs, drain_chunk)


def body(
    tokens, norm_gain, gate_weight, up_weight, down_weight, expert_ids, group_logits, pair_logits
):
    n_grp, n_fs, n_tp = (lax.axis_size(a) for a in ("grp", "fs", "tp"))
    n_x = n_tp // 2
    experts, block, hid = gate_weight.shape
    tok_rows, width = tokens.shape
    capacity = 5 * tok_rows * 2 // (4 * experts)
    cap = -(-capacity // 16) * 16
    vmem = pl.BlockSpec(memory_space=pltpu.VMEM)
    hbm = pl.BlockSpec(memory_space=pl.ANY)
    dma = pltpu.SemaphoreType.DMA
    matrix = jax.ShapeDtypeStruct((n_fs * block, hid), BF16)
    chunk = (n_fs, n_x, cap, width)
    sem_shapes = [
        (4,), (3,), (n_fs,), (n_fs,), (3, n_fs), (3, n_fs), (3, n_fs, n_grp), (3, n_fs, n_grp),
        (n_fs, n_x), (n_fs, n_x), (n_fs,), (n_fs,), (n_fs, n_x), (n_fs, n_x),
        (n_fs,), (n_fs,), (n_fs, n_x), (n_fs, n_x), (n_fs,), (n_fs,),
    ]
    mixed, *matrices = pl.pallas_call(
        functools.partial(exchange_kernel, n_grp, n_fs, n_tp, capacity),
        out_shape=(jax.ShapeDtypeStruct((tok_rows, width), BF16), matrix, matrix, matrix),
        in_specs=[vmem] * 5 + [hbm] * 3,
        out_specs=(vmem,) * 4,
        scratch_shapes=[
            pltpu.VMEM((n_fs, cap, width), BF16),
            pltpu.VMEM((3, n_fs, block, hid), F32),
            pltpu.VMEM((3, n_fs, block, hid), BF16),
            pltpu.VMEM((n_fs, cap, width), BF16),
            pltpu.VMEM((tok_rows, width), F32),
            pltpu.VMEM((n_tp, n_fs, cap, width), BF16),
            pltpu.VMEM((n_fs, cap, hid), BF16),
            pltpu.VMEM(chunk, F32),
            pltpu.VMEM(chunk, BF16),
            pltpu.VMEM(chunk, BF16),
            pltpu.VMEM(chunk, BF16),
            pltpu.VMEM(chunk, BF16),
            pltpu.VMEM((n_fs, cap, width), BF16),
        ] + [dma(s) for s in sem_shapes],
        compiler_params=pltpu.CompilerParams(
            collective_id=0, has_side_effects=True, vmem_limit_bytes=48 * 1024 * 1024
        ),
    )(
        tokens, norm_gain[:, None], expert_ids.T, group_logits.T, pair_logits.T,
        gate_weight, up_weight, down_weight,
    )
    return (mixed, *(m[None] for m in matrices))


def solution(mesh):
    placed = (
        P(("grp", "fs"), "tp"),
        P("fs"),
        P(None, "fs", "tp"),
        P(None, "fs", "tp"),
        P(None, "fs", "tp"),
        P(("grp", "fs"), None),
        P(("grp", "fs"), None),
        P(("grp", "fs"), None),
    )
    return jax.shard_map(
        body,
        mesh=mesh,
        in_specs=placed,
        out_specs=(
            P(("grp", "fs"), "tp"),
            P(("grp", "fs"), None, "tp"),
            P(("grp", "fs"), None, "tp"),
            P(("grp", "fs"), None, "tp"),
        ),
        check_vma=False,
    )
```
